32 devices in a mesh: sp: 16 (over z, y, x), tp: 2 (over core).
Axes of the slice: x: 2, y: 2, z: 4, core: 2. Of those that a mesh axis runs over, the one named last changes fastest.
Arguments:
- query_one: bfloat16 [2048, 1024], P('sp', 'tp'), may hold values from -85 to 85
- key_one: bfloat16 [2048, 1024], P('sp', 'tp'), may hold values from -6.5 to 6.5
- query_two: bfloat16 [2048, 1024], P('sp', 'tp'), may hold values from -85 to 85
- key_two: bfloat16 [2048, 1024], P('sp', 'tp'), may hold values from -6.5 to 6.5
- values: bfloat16 [2048, 2048], P('sp', 'tp'), may hold values from -6 to 6
- mix_weight: float32 [8], P('tp'), may hold values from 0.3 to 0.8
- head_gain: float32 [256], replicated, may hold values from 0.1 to 1.9
- residual: bfloat16 [2048, 2048], P(('sp', 'tp')), may hold values from -6 to 6
- out_weight: bfloat16 [2048, 2048], P('tp'), may hold values from -0.125 to 0.125
- norm_gain: float32 [2048], replicated, may hold values from 0.1 to 1.9
- lift_weight: bfloat16 [2048, 5632], P('sp', 'tp'), may hold values from -0.125 to 0.125
- gate_weight: bfloat16 [2048, 5632], P('sp', 'tp'), may hold values from -0.125 to 0.125
- conv_taps: float32 [3, 5632], P(None, 'tp'), may hold values from -3 to 3
- down_weight: bfloat16 [5632, 2048], P('tp'), may hold values from -0.078125 to 0.078125
Outputs:
- layer_out: bfloat16 [2048, 2048], P(('sp', 'tp'))
The draws below stay inside these ranges and needn't reach their ends.
All inputs are finite; a program needn't handle non-finite values.
Results may differ from the reference program's by a relative error of at most 0.015.
Values may be sent and summed in bfloat16 or wider, within the bound.
A program may use at most 128 MiB of HBM per device.

```python
import math
import jax
import jax.numpy as jnp
from jax import lax

D = 2048
HEADS = 8
HD = 128
VD = 256
FF = 5632
STRETCH = 64
WIDTH = 3
TOKENS = 2048
N_TP = 2


def drawn_pair(key, which):
    base = jax.random.fold_in(key, 71 + which)
    key_draw, query_draw = jax.random.split(base)
    keys = 1.3 * jnp.clip(jax.random.normal(key_draw, (TOKENS, HEADS * HD), jnp.float32), -5.0, 5.0)
    queries = 1.3 * jnp.clip(jax.random.normal(query_draw, (TOKENS, HEADS * HD), jnp.float32), -5.0, 5.0)
    return (queries, keys)


def draw_query_one(key, part):
    return drawn_pair(key, 0)[0].astype(jnp.bfloat16)


def draw_key_one(key, part):
    return drawn_pair(key, 0)[1].astype(jnp.bfloat16)


def draw_query_two(key, part):
    return drawn_pair(key, 1)[0].astype(jnp.bfloat16)


def draw_key_two(key, part):
    return drawn_pair(key, 1)[1].astype(jnp.bfloat16)


def levels(rng, extent, cuts, least, largest):
    def one(axis_at, parts):
        draws = jax.random.uniform(jax.random.fold_in(jax.random.fold_in(rng, 6), axis_at), (parts,), jnp.float32, least / len(cuts), largest / len(cuts))
        return jnp.repeat(jnp.exp(draws), extent[axis_at] // parts).reshape((-1,) + (1,) * (len(extent) - axis_at - 1))

    gain = one(*cuts[0])
    for cut in cuts[1:]:
        gain = gain * one(*cut)
    return gain


def centred(rng, dims, deviation, reach, cuts=(), kind=jnp.bfloat16):
    factor_of = levels(rng, dims, cuts, -0.22, 0.18) if cuts else 1.0
    drawn = jax.random.normal(rng, dims, jnp.float32) * deviation * factor_of
    return jnp.minimum(jnp.maximum(drawn, -reach), reach).astype(kind)


def setup_inputs(seed: int = 0) -> dict:
    key_list = jax.random.split(jax.random.key(seed), 15)
    return {
        "query_one": draw_query_one(jax.random.fold_in(key_list[14], 71), 0),
        "key_one": draw_key_one(jax.random.fold_in(key_list[14], 71), 0),
        "query_two": draw_query_two(jax.random.fold_in(key_list[14], 71), 0),
        "key_two": draw_key_two(jax.random.fold_in(key_list[14], 71), 0),
        "values": centred(key_list[4], (TOKENS, HEADS * VD), 1.0, 6.0, ((0, 16), (1, 2))),
        "mix_weight": jnp.clip(0.3 + 0.5 * jax.random.uniform(key_list[5], (HEADS,), jnp.float32) ** levels(key_list[5], (HEADS,), ((0, 2),), -0.2, 0.2), 0.3, 0.8),
        "head_gain": jnp.clip(1.0 + 0.18 * jax.random.normal(key_list[6], (VD,), jnp.float32), 0.1, 1.9),
        "residual": centred(key_list[7], (TOKENS, D), 1.0, 6.0, ((0, 32),)),
        "out_weight": centred(key_list[8], (HEADS * VD, D), (HEADS * VD) ** -0.5, 0.125, ((0, 2),)),
        "norm_gain": jnp.clip(1.0 + 0.18 * jax.random.normal(key_list[9], (D,), jnp.float32), 0.1, 1.9),
        "lift_weight": centred(key_list[10], (D, FF), D ** -0.5, 0.125, ((0, 16), (1, 2))),
        "gate_weight": centred(key_list[11], (D, FF), D ** -0.5, 0.125, ((0, 16), (1, 2))),
        "conv_taps": centred(key_list[12], (WIDTH, FF), 0.577, 3.0, ((1, 2),), jnp.float32),
        "down_weight": centred(key_list[13], (FF, D), FF ** -0.5, 0.078125, ((0, 2),)),
    }


epsilon = 1e-06
masked_score = -1e+30

def attend_block(first_q, first_k, second_q, second_k, vals, mix_weight, head_gain, start, block_rows):
    scale_factor = HD ** (-0.5)
    q_pos = start + lax.iota(jnp.int32, block_rows)
    k_pos = lax.iota(jnp.int32, TOKENS)
    visible = k_pos[None, :] // STRETCH <= q_pos[:, None] // STRETCH

    def one_map(queries, keys):
        scores = jnp.einsum('thd,shd->hts', queries, keys) * scale_factor
        scores = jnp.where(visible[None], scores, masked_score)
        peak = lax.optimization_barrier(jnp.max(scores, axis=-1, keepdims=True))
        weights = jnp.where(visible[None], jnp.exp(scores - peak), 0.0)
        total = lax.optimization_barrier(jnp.sum(weights, axis=-1))
        rounded = lax.optimization_barrier(weights.astype(jnp.bfloat16))
        acc = jnp.einsum('hts,she->hte', rounded.astype(jnp.float32), vals)
        return acc / total[..., None]
    mixed = one_map(first_q, first_k) - mix_weight[:, None, None] * one_map(second_q, second_k)
    normed = mixed * lax.rsqrt(lax.optimization_barrier(jnp.mean(mixed * mixed, axis=-1, keepdims=True)) + epsilon) * head_gain
    return jnp.transpose(normed.astype(jnp.bfloat16), (1, 0, 2))

def reference(query_one, key_one, query_two, key_two, values, mix_weight, head_gain, residual, out_weight, norm_gain, lift_weight, gate_weight, conv_taps, down_weight):
    val_width = 2 * HD
    block_rows = math.gcd(TOKENS, 512)
    blocks = TOKENS // block_rows
    q_one = query_one.astype(jnp.float32).reshape(TOKENS, HEADS, HD)
    q_two = query_two.astype(jnp.float32).reshape(TOKENS, HEADS, HD)
    k_one = key_one.astype(jnp.float32).reshape(TOKENS, HEADS, HD)
    k_two = key_two.astype(jnp.float32).reshape(TOKENS, HEADS, HD)
    vals = values.astype(jnp.float32).reshape(TOKENS, HEADS, val_width)

    def per_block(index):
        start = (index * block_rows).astype(jnp.int32)
        first_q = lax.dynamic_slice_in_dim(q_one, start, block_rows, 0)
        second_q = lax.dynamic_slice_in_dim(q_two, start, block_rows, 0)
        return attend_block(first_q, k_one, second_q, k_two, vals, mix_weight, head_gain, start, block_rows)
    head_out = lax.map(per_block, jnp.arange(blocks, dtype=jnp.int32))
    head_out = head_out.reshape(TOKENS, HEADS * val_width)
    group = HEADS * val_width // N_TP
    attended = jnp.zeros((TOKENS, D), jnp.float32)
    for index in range(N_TP):
        partial_sum = jnp.dot(head_out[:, index * group:(index + 1) * group], out_weight[index * group:(index + 1) * group], preferred_element_type=jnp.float32)
        attended = attended + partial_sum.astype(jnp.bfloat16).astype(jnp.float32)
    stream = residual.astype(jnp.float32) + attended
    normed = (stream * lax.rsqrt(lax.optimization_barrier(jnp.mean(stream * stream, axis=-1, keepdims=True)) + epsilon) * norm_gain).astype(jnp.bfloat16)
    lifted = jnp.dot(normed, lift_weight, preferred_element_type=jnp.float32).astype(jnp.bfloat16)
    gated = jnp.dot(normed, gate_weight, preferred_element_type=jnp.float32).astype(jnp.bfloat16)
    padded = jnp.concatenate([jnp.zeros((WIDTH - 1, FF), jnp.float32), gated.astype(jnp.float32)], axis=0)
    conv = jnp.zeros((TOKENS, FF), jnp.float32)
    for index in range(WIDTH):
        conv = conv + conv_taps[index] * padded[index:index + TOKENS]
    hidden = (jax.nn.silu(conv) * lifted.astype(jnp.float32)).astype(jnp.bfloat16)
    units = FF // N_TP
    mixer = jnp.zeros((TOKENS, D), jnp.float32)
    for index in range(N_TP):
        partial_sum = jnp.dot(hidden[:, index * units:(index + 1) * units], down_weight[index * units:(index + 1) * units], preferred_element_type=jnp.float32)
        mixer = mixer + partial_sum.astype(jnp.bfloat16).astype(jnp.float32)
    return (stream + mixer).astype(jnp.bfloat16)
```

```python
import functools

import jax
import jax.numpy as jnp
from jax import lax
from jax.experimental import pallas as pl
from jax.experimental.pallas import tpu as pltpu
from jax.sharding import PartitionSpec as P

HD = 128
STRETCH = 64
WIDTH = 3


epsilon = 1e-06
masked_score = -1e30


def passed_along(block, axis, distance):
    devices = range(lax.axis_size(axis))
    route = [(i - distance, i) for i in devices if i - distance in devices]
    return lax.ppermute(block, axis, route)


def update_map(peak, total, acc, queries, keys, vals, visible):
    scores = jnp.einsum("thd,shd->hts", queries, keys, preferred_element_type=jnp.float32) * HD ** (
        -0.5
    )
    scores = jnp.where(visible[None], scores, masked_score)
    new_peak = jnp.maximum(peak, jnp.max(scores, axis=-1))
    weights = jnp.where(visible[None], jnp.exp(scores - new_peak[..., None]), 0.0)
    total = jnp.sum(weights, axis=-1)
    acc = jnp.einsum(
        "hts,she->hte", weights.astype(jnp.bfloat16), vals, preferred_element_type=jnp.float32
    )
    return (new_peak, total, acc)


def on_device(
    query_one,
    key_one,
    query_two,
    key_two,
    values,
    mix_weight,
    head_gain,
    residual,
    out_weight,
    norm_gain,
    lift_weight,
    gate_weight,
    conv_taps,
    down_weight,
):
    tok_local = query_one.shape[0]
    heads_local = mix_weight.shape[0]
    val_width = values.shape[1] // heads_local
    model_width = residual.shape[1]
    offset = lax.axis_index("sp") * tok_local
    q_pos = offset + lax.iota(jnp.int32, tok_local)
    q_one = query_one.reshape(tok_local, heads_local, HD)
    q_two = query_two.reshape(tok_local, heads_local, HD)
    start_peak = jnp.full((heads_local, tok_local), masked_score, jnp.float32)
    start_total = jnp.zeros((heads_local, tok_local), jnp.float32)
    start_acc = jnp.zeros((heads_local, tok_local, val_width), jnp.float32)
    initial = (start_peak, start_total, start_acc, start_peak, start_total, start_acc)
    first_keys = lax.all_gather(key_one, "sp", axis=0, tiled=True)
    second_keys = lax.all_gather(key_two, "sp", axis=0, tiled=True)
    piece_vals = lax.all_gather(values, "sp", axis=0, tiled=True)
    count = first_keys.shape[0]
    k_pos = lax.iota(jnp.int32, count)
    visible = k_pos[None, :] // STRETCH <= q_pos[:, None] // STRETCH
    first_keys = first_keys.reshape(count, heads_local, HD)
    second_keys = second_keys.reshape(count, heads_local, HD)
    piece_vals = piece_vals.reshape(count, heads_local, val_width)
    first = update_map(initial[0], initial[1], initial[2], q_one, first_keys, piece_vals, visible)
    second = update_map(initial[3], initial[4], initial[5], q_two, second_keys, piece_vals, visible)
    state = first + second
    mixed = (
        state[2] / state[1][..., None] - mix_weight[:, None, None] * state[5] / state[4][..., None]
    )
    head_out = (
        mixed * lax.rsqrt(jnp.mean(mixed * mixed, axis=-1, keepdims=True) + epsilon) * head_gain
    ).astype(jnp.bfloat16)
    out_heads = out_weight.reshape(heads_local, val_width, model_width)
    piece = head_out
    attended = lax.psum_scatter(
        jnp.einsum("hte,hed->td", piece, out_heads, preferred_element_type=jnp.float32).astype(
            jnp.bfloat16
        ),
        "tp",
        scatter_dimension=0,
        tiled=True,
    ).astype(jnp.float32)
    stream = residual.astype(jnp.float32) + attended
    normed = (
        stream * lax.rsqrt(jnp.mean(stream * stream, axis=-1, keepdims=True) + epsilon) * norm_gain
    ).astype(jnp.bfloat16)
    whole_rows = lax.all_gather(normed, "tp", axis=0, tiled=True)
    lift_pre = jnp.dot(
        whole_rows,
        lax.all_gather(lift_weight, "sp", axis=0, tiled=True),
        preferred_element_type=jnp.float32,
    )
    gate_pre = jnp.dot(
        whole_rows,
        lax.all_gather(gate_weight, "sp", axis=0, tiled=True),
        preferred_element_type=jnp.float32,
    )
    lifted = lift_pre.astype(jnp.bfloat16)
    gated = gate_pre.astype(jnp.bfloat16)
    prior = passed_along(gated[tok_local - (WIDTH - 1) :], "sp", 1)
    extended = jnp.concatenate([prior, gated], axis=0).astype(jnp.float32)
    conv = conv_taps[0] * extended[0:tok_local]
    for index in range(1, WIDTH):
        conv = conv + conv_taps[index] * extended[index : index + tok_local]
    hidden = (jax.nn.silu(conv) * lifted.astype(jnp.float32)).astype(jnp.bfloat16)
    piece = hidden
    mixer = lax.psum_scatter(
        jnp.dot(piece, down_weight, preferred_element_type=jnp.float32).astype(jnp.bfloat16),
        "tp",
        scatter_dimension=0,
        tiled=True,
    ).astype(jnp.float32)
    return (stream + mixer).astype(jnp.bfloat16)

MESH = pl.DeviceIdType.MESH


def remote(src, dst, send_sem, recv_sem, sp, tp):
    return pltpu.make_async_remote_copy(
        src_ref=src,
        dst_ref=dst,
        send_sem=send_sem,
        recv_sem=recv_sem,
        device_id=(sp, tp),
        device_id_type=MESH,
    )


def block_of(index, size):
    return pl.ds(pl.multiple_of(index * size, size), size)


def layer_kernel(
    plane, planes, width,
    q1, k1, q2, k2, v, lift, gate, mix_weight, head_gain, out_hbm, residual_hbm, gain, taps, down_hbm,
    out,
    q_all, kv_all, head_out, heads, part, part_in, tail, out_weight, residual, stream, piece_out, piece_in,
    lift_all, gate_all, held, normed, gated, hidden, units, total,
    own_sem, a_send, a_recv, k_send, k_recv, w_send, w_recv, g_send, g_recv, l_sem,
    b_own, b_send, b_recv, t_send, t_recv, n_send, n_recv, f_send, f_recv,
    h_send, h_recv, hf_send, hf_recv, u_send, u_recv, y_send, y_recv,
):
    sp, tp = lax.axis_index("sp"), lax.axis_index("tp")
    z, p = sp // plane, sp % plane
    other = 1 - tp
    tok = q1.shape[0]
    half = tok // 2
    val = 2 * HD
    span = plane * tok
    tiles = lift.shape[1] // 128
    model = out_weight.shape[1]
    pad = normed.shape[1] - tok
    before, after = (p + plane - 1) % plane, (p + 1) % plane
    zone = z + (p + 1) // plane
    weights = ((lift, lift_all), (gate, gate_all))

    square = plane == 4
    direct = (1, 2) if square else range(1, plane)

    def flip(index, e):
        return {0: index, 1: index + 1 - 2 * (index % 2), 2: (index + 2) % 4, 3: 3 - index}[e]

    def to_chip(e):
        return flip(p, e) if square else (p + e) % plane

    def from_chip(e):
        return flip(p, e) if square else (p + plane - e) % plane

    def to_plane(d):
        return flip(z, d) if planes == 4 else (z + d) % planes

    def from_plane(d):
        return flip(z, d) if planes == 4 else (z + planes - d) % planes

    peers = (
        [(z * plane + (p + d) % plane, tp) for d in range(1, plane)]
        + [((z + d) % planes * plane + p, tp) for d in range(1, planes)]
        + [(sp, other)]
    )
    barrier = pltpu.get_barrier_semaphore()
    for peer in peers:
        pl.semaphore_signal(barrier, inc=1, device_id=peer, device_id_type=MESH)

    @pl.when(tp == 1)
    def _():
        for s in range(planes):
            pl.semaphore_signal(
                barrier, inc=1, device_id=(s * plane + before, 1), device_id_type=MESH
            )

    def piece(head, row):
        h1, h2 = block_of(head, HD), block_of(head, val)
        rows, own_rows = block_of(row * plane + p, tok), block_of(row, tok)
        return [
            (k1.at[:, h1], kv_all.at[rows, 0:HD]),
            (k2.at[:, h1], kv_all.at[rows, HD : 2 * HD]),
            (v.at[:, h2], kv_all.at[rows, 2 * HD : 4 * HD]),
            (q1.at[:, h1], q_all.at[own_rows, 0:HD]),
            (q2.at[:, h1], q_all.at[own_rows, HD : 2 * HD]),
        ]

    def units_of(index):
        return pl.ds(pl.multiple_of(index * tiles // planes * 128, 128), width)

    own = [
        pltpu.make_async_copy(src, dst, own_sem.at[n]) for n, (src, dst) in enumerate(piece(z, z))
    ]
    own_weights = [
        pltpu.make_async_copy(src.at[:, units_of(z)], dst.at[block_of(sp, tok), :], own_sem.at[5 + m])
        for m, (src, dst) in enumerate(weights)
    ]
    loads = [
        pltpu.make_async_copy(out_hbm, out_weight, own_sem.at[7]),
        pltpu.make_async_copy(residual_hbm, residual, own_sem.at[8]),
    ]

    def load(s):
        first = s * tiles // planes * 128
        return pltpu.make_async_copy(down_hbm.at[first : first + width, :], held.at[s], l_sem.at[s])

    for copy in own:
        copy.start()
    started = []

    def send(copy):
        copy.start()
        started.append(copy)

    pl.semaphore_wait(barrier, len(peers) + planes * tp)

    def exchange(which):
        for d in range(1, planes):
            pairs = piece(to_plane(d), z)
            for n in which:
                src, dst = pairs[n]
                send(remote(src, dst, a_send.at[d, n], a_recv.at[d, n], to_plane(d) * plane + p, tp))

    def exchanged(d, which):
        pairs = piece(z, from_plane(d))
        for n in which:
            src, dst = pairs[n]
            remote(src, dst, a_send.at[d, n], a_recv.at[d, n], sp, other).wait_recv()

    def kv_block(d, m, chip):
        rows = block_of(from_plane(d) * plane + chip, tok)
        return kv_all.at[rows, m * val : (m + 1) * val]

    def weight_block(d, m, chip):
        return weights[m][1].at[block_of(from_plane(d) * plane + chip, tok), :]

    kv = (kv_block, k_send, k_recv)
    wt = (weight_block, g_send, g_recv)

    def spread(kind, d, m, src=None):
        block_at, sends, recvs = kind
        block = block_at(d, m, p)
        for e in direct:
            send(
                remote(
                    block if src is None else src, block, sends.at[d, e, m], recvs.at[d, e, m],
                    z * plane + to_chip(e), tp,
                )
            )

    def arrived(kind, d, e, m):
        block_at, sends, recvs = kind
        block = block_at(d, m, from_chip(e))
        remote(block, block, sends.at[d, e, m], recvs.at[d, e, m], sp, other).wait_recv()

    def relay(kind, d, m):
        block_at, sends, recvs = kind
        for e in direct:
            arrived(kind, d, e, m)
            if square and e == m + 1:
                block = block_at(d, m, from_chip(e))
                send(
                    remote(
                        block, block, sends.at[d, 3, m], recvs.at[d, 3, m],
                        z * plane + to_chip(3 - e), tp,
                    )
                )

    def settle(kind, d, m):
        if square:
            arrived(kind, d, 3, m)

    def send_weights(m):
        for d in range(1, planes):
            src, dst = weights[m]
            send(
                remote(
                    src.at[:, units_of(to_plane(d))], dst.at[block_of(sp, tok), :],
                    w_send.at[d, m], w_recv.at[d, m], to_plane(d) * plane + p, tp,
                )
            )

    def share_weights(d, m):
        if d == 0:
            spread(wt, d, m, weights[m][0].at[:, units_of(z)])
        else:
            block = weight_block(d, m, p)
            remote(block, block, w_send.at[d, m], w_recv.at[d, m], sp, other).wait_recv()
            spread(wt, d, m)

    exchange((0, 1, 2))
    for copy in own[:3]:
        copy.wait()
    for m in range(2):
        spread(kv, 0, m)
    exchange((3, 4))
    share_weights(0, 0)
    send_weights(0)
    for copy in own_weights + loads:
        copy.start()
    for s in range(planes):
        load(s).start()
    for d in range(1, planes):
        exchanged(d, (0, 1, 2))
        for m in range(2):
            spread(kv, d, m)
        for m in range(2):
            relay(kv, d - 1, m)
    for m in range(2):
        relay(kv, planes - 1, m)
    share_weights(0, 1)
    relay(wt, 0, 0)
    for copy in own[3:]:
        copy.wait()
    for d in range(1, planes):
        exchanged(d, (3, 4))
    for d in range(planes):
        for m in range(2):
            settle(kv, d, m)

    for s in range(planes):
        rows, count = slice(s * tok, (s + 1) * tok), (s + 1) * span
        mixed = None
        for m in range(2):
            scores = lax.dot_general(
                q_all[rows, m * HD : (m + 1) * HD],
                kv_all[0:count, m * HD : (m + 1) * HD],
                (((1,), (1,)), ((), ())),
                preferred_element_type=jnp.float32,
            ) * HD ** (-0.5)
            k_pos = lax.broadcasted_iota(jnp.int32, (tok, span), 1)
            q_pos = p * tok + lax.broadcasted_iota(jnp.int32, (tok, span), 0)
            visible = lax.div(k_pos, STRETCH) <= lax.div(q_pos, STRETCH)
            last = jnp.where(visible, scores[:, count - span :], masked_score)
            scores = jnp.concatenate([scores[:, : count - span], last], axis=1) if s else last
            peak = jnp.max(scores, axis=-1, keepdims=True)
            terms = jnp.exp(scores - peak)
            sums = jnp.sum(terms, axis=-1, keepdims=True)
            acc = jnp.dot(
                terms.astype(jnp.bfloat16),
                kv_all[0:count, 2 * HD : 4 * HD],
                preferred_element_type=jnp.float32,
            )
            if m == 0:
                mixed = acc / sums
            else:
                mixed = mixed - mix_weight[z] * acc / sums
        scale = lax.rsqrt(jnp.mean(mixed * mixed, axis=-1, keepdims=True) + epsilon)
        head_out[s] = (mixed * scale * head_gain[...]).astype(jnp.bfloat16)

        @pl.when(z != s)
        def _():
            remote(
                head_out.at[s], heads.at[z], b_send.at[s], b_recv.at[z], s * plane + p, tp
            ).start()

        @pl.when(z == s)
        def _():
            pltpu.make_async_copy(head_out.at[s], heads.at[z], b_own).start()

    send_weights(1)
    for m in range(2):
        if m == 0:
            for d in range(1, planes):
                share_weights(d, 0)
        else:
            relay(wt, 0, 1)
    for d in range(1, planes):
        relay(wt, d, 0)
    for s in range(planes):

        @pl.when(z != s)
        def _():
            remote(
                heads.at[s], heads.at[s], b_send.at[s], b_recv.at[s], sp, other
            ).wait_recv()

        @pl.when(z == s)
        def _():
            pltpu.make_async_copy(head_out.at[s], heads.at[s], b_own).wait()

    for copy in loads:
        copy.wait()
    columns = 512

    def product(which, at):
        sums = None
        for h in range(planes):
            term = jnp.dot(
                heads[h, block_of(which, half), :],
                out_weight[h * val : (h + 1) * val, at : at + columns],
                preferred_element_type=jnp.float32,
            )
            sums = term if sums is None else sums + term
        return sums.astype(jnp.bfloat16)

    for at in range(0, model, columns):
        part[:, at : at + columns] = product(other, at)
    swap = remote(part, part_in, t_send, t_recv, sp, other)
    send(swap)
    for at in range(0, model, columns):
        stream[:, at : at + columns] = product(tp, at).astype(jnp.float32)
    swap.wait_recv()
    whole = residual[...].astype(jnp.float32) + (stream[...] + part_in[...].astype(jnp.float32))
    stream[...] = whole
    scaled = whole * lax.rsqrt(jnp.mean(whole * whole, axis=-1, keepdims=True) + epsilon) * gain[...]

    def tokens(s, which):
        return normed.at[s, pl.ds(pl.multiple_of(pad + which * half, 8), half), :]

    normed[z, pl.ds(pl.multiple_of(pad + tp * half, 8), half), :] = scaled.astype(jnp.bfloat16)
    tail[...] = scaled[half - pad :, :].astype(jnp.bfloat16)
    mine = tokens(z, tp)
    for d in range(1, planes):
        send(remote(mine, mine, n_send.at[d], n_recv.at[d], to_plane(d) * plane + p, tp))
    send(remote(mine, mine, f_send.at[0], f_recv.at[0], sp, other))

    @pl.when(jnp.logical_and(tp == 1, zone < planes))
    def _():
        for s in range(planes):
            remote(
                tail, normed.at[zone, 0:pad, :], h_send.at[s], h_recv.at[zone], s * plane + after, 1
            ).start()

    for d in range(1, planes):
        share_weights(d, 1)
    for d in range(1, planes):
        theirs = tokens(from_plane(d), tp)
        remote(theirs, theirs, n_send.at[d], n_recv.at[d], sp, other).wait_recv()
        send(remote(theirs, theirs, f_send.at[d], f_recv.at[d], sp, other))
    for s in range(planes):
        rows = normed.at[s, 0:pad, :]

        @pl.when(s * plane + p > 0)
        def _():
            @pl.when(tp == 1)
            def _():
                remote(rows, rows, h_send.at[s], h_recv.at[s], sp, other).wait_recv()
                remote(rows, rows, hf_send.at[s], hf_recv.at[s], sp, other).start()

            @pl.when(tp == 0)
            def _():
                remote(rows, rows, hf_send.at[s], hf_recv.at[s], sp, other).wait_recv()

        @pl.when(s * plane + p == 0)
        def _():
            normed[s, 0:pad, :] = jnp.zeros((pad, model), jnp.bfloat16)

    for d in range(1, planes):
        relay(wt, d, 1)
    for copy in own_weights:
        copy.wait()
    for m in range(2):
        for d in range(planes):
            settle(wt, d, m)

    first = z * tiles // planes * 128
    mine_units = (z + 1) * tiles // planes * 128 - first
    chunk = 256 if width % 256 == 0 else 128
    for d in range(planes):
        s = from_plane(d)
        theirs = tokens(s, other)
        remote(theirs, theirs, f_send.at[d], f_recv.at[d], sp, other).wait_recv()

        @pl.loop(0, width // chunk)
        def _(at):
            here = block_of(at, chunk)
            gated[...] = (
                jnp.dot(normed[s], gate_all[:, here], preferred_element_type=jnp.float32)
                .astype(jnp.bfloat16)
                .astype(jnp.float32)
            )
            lifted = (
                jnp.dot(normed[s, pad:, :], lift_all[:, here], preferred_element_type=jnp.float32)
                .astype(jnp.bfloat16)
                .astype(jnp.float32)
            )
            lanes = pl.ds(pl.multiple_of(first + at * chunk, 128), chunk)
            conv = None
            for index in range(WIDTH):
                start = pad - (WIDTH - 1) + index
                term = taps[index : index + 1, lanes] * gated[start : start + tok, :]
                conv = term if conv is None else conv + term
            inside = at * chunk + lax.broadcasted_iota(jnp.int32, (tok, chunk), 1) < mine_units
            hidden[s, :, here] = jnp.where(inside, jax.nn.silu(conv) * lifted, 0.0).astype(
                jnp.bfloat16
            )

        if d:
            send(remote(hidden.at[s], units.at[z], u_send.at[d], u_recv.at[d], s * plane + p, tp))

    for d in range(planes):
        s = from_plane(d)
        if d == 0:
            for n in range(planes):
                load(n).wait()
        else:
            remote(units.at[s], units.at[s], u_send.at[d], u_recv.at[d], sp, other).wait_recv()

        @pl.loop(0, model // columns)
        def _(at):
            here = block_of(at, columns)
            block = hidden[s] if d == 0 else units[s]
            term = jnp.dot(block, held[s, :, here], preferred_element_type=jnp.float32)
            total[:, here] = term if d == 0 else total[:, here] + term

    piece_out[...] = total[block_of(other, half), :].astype(jnp.bfloat16)
    swap = remote(piece_out, piece_in, y_send, y_recv, sp, other)
    send(swap)
    near = total[block_of(tp, half), :].astype(jnp.bfloat16).astype(jnp.float32)
    swap.wait_recv()
    out[...] = (stream[...] + (near + piece_in[...].astype(jnp.float32))).astype(out.dtype)

    for s in range(planes):

        @pl.when(z != s)
        def _():
            remote(
                head_out.at[s], heads.at[z], b_send.at[s], b_recv.at[z], s * plane + p, tp
            ).wait_send()

        @pl.when(jnp.logical_and(tp == 1, s * plane + p > 0))
        def _():
            rows = normed.at[s, 0:pad, :]
            remote(rows, rows, hf_send.at[s], hf_recv.at[s], sp, other).wait_send()

        @pl.when(jnp.logical_and(tp == 1, zone < planes))
        def _():
            remote(
                tail, normed.at[s, 0:pad, :], h_send.at[s], h_recv.at[s], s * plane + after, 1
            ).wait_send()

    for copy in started:
        copy.wait_send()


def shorter_routes(
    plane, planes,
    query_one, key_one, query_two, key_two, values, mix_weight, head_gain, residual, out_weight,
    norm_gain, lift_weight, gate_weight, conv_taps, down_weight,
):
    bf16, f32 = jnp.bfloat16, jnp.float32
    tok = query_one.shape[0]
    model = residual.shape[1]
    val = 2 * HD
    tiles = lift_weight.shape[1] // 128
    width = -(-tiles // planes) * 128
    chunk = 256 if width % 256 == 0 else 128
    count = planes * plane * tok
    half = tok // 2
    pad = 8
    dma = pltpu.SemaphoreType.DMA
    anywhere = pl.BlockSpec(memory_space=pl.ANY)
    local = pl.BlockSpec(memory_space=pltpu.VMEM)
    scalars = pl.BlockSpec(memory_space=pltpu.SMEM)
    each = dma((planes,))
    return pl.pallas_call(
        functools.partial(layer_kernel, plane, planes, width),
        out_shape=jax.ShapeDtypeStruct((half, model), bf16),
        in_specs=[anywhere] * 7 + [scalars, local, anywhere, anywhere, local, local, anywhere],
        out_specs=local,
        scratch_shapes=[
            pltpu.VMEM((planes * tok, 2 * HD), bf16),
            pltpu.VMEM((count, 4 * HD), bf16),
            pltpu.VMEM((planes, tok, val), bf16),
            pltpu.VMEM((planes, tok, val), bf16),
            pltpu.VMEM((half, model), bf16),
            pltpu.VMEM((half, model), bf16),
            pltpu.VMEM((pad, model), bf16),
            pltpu.VMEM(out_weight.shape, bf16),
            pltpu.VMEM(residual.shape, bf16),
            pltpu.VMEM((half, model), f32),
            pltpu.VMEM((half, model), bf16),
            pltpu.VMEM((half, model), bf16),
            pltpu.VMEM((count, width), bf16),
            pltpu.VMEM((count, width), bf16),
            pltpu.VMEM((planes, width, model), bf16),
            pltpu.VMEM((planes, pad + tok, model), bf16),
            pltpu.VMEM((pad + tok, chunk), f32),
            pltpu.VMEM((planes, tok, width), bf16),
            pltpu.VMEM((planes, tok, width), bf16),
            pltpu.VMEM((tok, model), f32),
            dma((9,)), dma((planes, 5)), dma((planes, 5)),
            dma((planes, plane, 2)), dma((planes, plane, 2)),
            dma((planes, 2)), dma((planes, 2)),
            dma((planes, plane, 2)), dma((planes, plane, 2)), each,
            dma, each, each, dma, dma, each, each, each, each,
            each, each, each, each, each, each, dma, dma,
        ],
        compiler_params=pltpu.CompilerParams(
            collective_id=0, has_side_effects=True, vmem_limit_bytes=62 << 20
        ),
        name="layer",
    )(
        query_one, key_one, query_two, key_two, values, lift_weight, gate_weight, mix_weight,
        head_gain.reshape(1, val), out_weight, residual, norm_gain.reshape(1, model), conv_taps,
        down_weight,
    )


def any_route(*arrays):
    tok, heads, ff = arrays[0].shape[0], arrays[5].shape[0], arrays[10].shape[1]
    devices, groups = lax.axis_size("sp"), lax.axis_size("tp")
    fits = (
        groups == 2 and heads > 1 and devices > heads and devices % heads == 0
        and ff % 128 == 0 and tok % 128 == 0 and WIDTH <= 9
        and arrays[10].shape[0] == tok
    )
    if fits:
        return shorter_routes(devices // heads, heads, *arrays)
    return on_device(*arrays)


def solution(mesh):
    return jax.shard_map(
        any_route,
        mesh=mesh,
        in_specs=(
            P("sp", "tp"),
            P("sp", "tp"),
            P("sp", "tp"),
            P("sp", "tp"),
            P("sp", "tp"),
            P("tp"),
            P(),
            P(("sp", "tp"), None),
            P("tp", None),
            P(),
            P("sp", "tp"),
            P("sp", "tp"),
            P(None, "tp"),
            P("tp", None),
        ),
        out_specs=P(("sp", "tp"), None),
        check_vma=False,
    )
```

```python
import functools

import jax
import jax.numpy as jnp
from jax import lax
from jax.experimental import pallas as pl
from jax.experimental.pallas import tpu as pltpu
from jax.sharding import PartitionSpec as P

HD = 128
STRETCH = 64
WIDTH = 3


epsilon = 1e-06
masked_score = -1e30


def passed_along(block, axis, distance):
    devices = range(lax.axis_size(axis))
    route = [(i - distance, i) for i in devices if i - distance in devices]
    return lax.ppermute(block, axis, route)


def update_map(peak, total, acc, queries, keys, vals, visible):
    scores = jnp.einsum("thd,shd->hts", queries, keys, preferred_element_type=jnp.float32) * HD ** (
        -0.5
    )
    scores = jnp.where(visible[None], scores, masked_score)
    new_peak = jnp.maximum(peak, jnp.max(scores, axis=-1))
    weights = jnp.where(visible[None], jnp.exp(scores - new_peak[..., None]), 0.0)
    total = jnp.sum(weights, axis=-1)
    acc = jnp.einsum(
        "hts,she->hte", weights.astype(jnp.bfloat16), vals, preferred_element_type=jnp.float32
    )
    return (new_peak, total, acc)


def on_device(
    query_one,
    key_one,
    query_two,
    key_two,
    values,
    mix_weight,
    head_gain,
    residual,
    out_weight,
    norm_gain,
    lift_weight,
    gate_weight,
    conv_taps,
    down_weight,
):
    tok_local = query_one.shape[0]
    heads_local = mix_weight.shape[0]
    val_width = values.shape[1] // heads_local
    model_width = residual.shape[1]
    offset = lax.axis_index("sp") * tok_local
    q_pos = offset + lax.iota(jnp.int32, tok_local)
    q_one = query_one.reshape(tok_local, heads_local, HD)
    q_two = query_two.reshape(tok_local, heads_local, HD)
    start_peak = jnp.full((heads_local, tok_local), masked_score, jnp.float32)
    start_total = jnp.zeros((heads_local, tok_local), jnp.float32)
    start_acc = jnp.zeros((heads_local, tok_local, val_width), jnp.float32)
    initial = (start_peak, start_total, start_acc, start_peak, start_total, start_acc)
    first_keys = lax.all_gather(key_one, "sp", axis=0, tiled=True)
    second_keys = lax.all_gather(key_two, "sp", axis=0, tiled=True)
    piece_vals = lax.all_gather(values, "sp", axis=0, tiled=True)
    count = first_keys.shape[0]
    k_pos = lax.iota(jnp.int32, count)
    visible = k_pos[None, :] // STRETCH <= q_pos[:, None] // STRETCH
    first_keys = first_keys.reshape(count, heads_local, HD)
    second_keys = second_keys.reshape(count, heads_local, HD)
    piece_vals = piece_vals.reshape(count, heads_local, val_width)
    first = update_map(initial[0], initial[1], initial[2], q_one, first_keys, piece_vals, visible)
    second = update_map(initial[3], initial[4], initial[5], q_two, second_keys, piece_vals, visible)
    state = first + second
    mixed = (
        state[2] / state[1][..., None] - mix_weight[:, None, None] * state[5] / state[4][..., None]
    )
    head_out = (
        mixed * lax.rsqrt(jnp.mean(mixed * mixed, axis=-1, keepdims=True) + epsilon) * head_gain
    ).astype(jnp.bfloat16)
    out_heads = out_weight.reshape(heads_local, val_width, model_width)
    piece = head_out
    attended = lax.psum_scatter(
        jnp.einsum("hte,hed->td", piece, out_heads, preferred_element_type=jnp.float32).astype(
            jnp.bfloat16
        ),
        "tp",
        scatter_dimension=0,
        tiled=True,
    ).astype(jnp.float32)
    stream = residual.astype(jnp.float32) + attended
    normed = (
        stream * lax.rsqrt(jnp.mean(stream * stream, axis=-1, keepdims=True) + epsilon) * norm_gain
    ).astype(jnp.bfloat16)
    whole_rows = lax.all_gather(normed, "tp", axis=0, tiled=True)
    lift_pre = jnp.dot(
        whole_rows,
        lax.all_gather(lift_weight, "sp", axis=0, tiled=True),
        preferred_element_type=jnp.float32,
    )
    gate_pre = jnp.dot(
        whole_rows,
        lax.all_gather(gate_weight, "sp", axis=0, tiled=True),
        preferred_element_type=jnp.float32,
    )
    lifted = lift_pre.astype(jnp.bfloat16)
    gated = gate_pre.astype(jnp.bfloat16)
    prior = passed_along(gated[tok_local - (WIDTH - 1) :], "sp", 1)
    extended = jnp.concatenate([prior, gated], axis=0).astype(jnp.float32)
    conv = conv_taps[0] * extended[0:tok_local]
    for index in range(1, WIDTH):
        conv = conv + conv_taps[index] * extended[index : index + tok_local]
    hidden = (jax.nn.silu(conv) * lifted.astype(jnp.float32)).astype(jnp.bfloat16)
    piece = hidden
    mixer = lax.psum_scatter(
        jnp.dot(piece, down_weight, preferred_element_type=jnp.float32).astype(jnp.bfloat16),
        "tp",
        scatter_dimension=0,
        tiled=True,
    ).astype(jnp.float32)
    return (stream + mixer).astype(jnp.bfloat16)

MESH = pl.DeviceIdType.MESH


def remote(src, dst, send_sem, recv_sem, sp, tp):
    return pltpu.make_async_remote_copy(
        src_ref=src,
        dst_ref=dst,
        send_sem=send_sem,
        recv_sem=recv_sem,
        device_id=(sp, tp),
        device_id_type=MESH,
    )


def block_of(index, size):
    return pl.ds(pl.multiple_of(index * size, size), size)


def layer_kernel(
    plane, planes, width,
    q1, k1, q2, k2, v, lift, gate, mix_weight, head_gain, out_hbm, residual_hbm, gain, taps, down_hbm,
    out,
    q_all, kv_all, head_out, heads, part, part_in, tail, out_weight, residual, stream, piece_out, piece_in,
    lift_all, gate_all, held, normed, gated, hidden, units, total,
    own_sem, a_send, a_recv, k_send, k_recv, w_send, w_recv, g_send, g_recv, l_sem,
    b_own, b_send, b_recv, t_send, t_recv, n_send, n_recv, f_send, f_recv,
    h_send, h_recv, hf_send, hf_recv, u_send, u_recv, y_send, y_recv,
):
    sp, tp = lax.axis_index("sp"), lax.axis_index("tp")
    z, p = sp // plane, sp % plane
    other = 1 - tp
    tok = q1.shape[0]
    half = tok // 2
    val = 2 * HD
    span = plane * tok
    tiles = lift.shape[1] // 128
    model = out_weight.shape[1]
    pad = normed.shape[1] - tok
    before, after = (p + plane - 1) % plane, (p + 1) % plane
    zone = z + (p + 1) // plane
    weights = ((lift, lift_all), (gate, gate_all))
    widths = sorted({(s + 1) * tiles // planes - s * tiles // planes for s in range(planes)})

    square = plane == 4
    direct = (1, 2) if square else range(1, plane)

    def flip(index, e):
        return {0: index, 1: index + 1 - 2 * (index % 2), 2: (index + 2) % 4, 3: 3 - index}[e]

    def to_chip(e):
        return flip(p, e) if square else (p + e) % plane

    def from_chip(e):
        return flip(p, e) if square else (p + plane - e) % plane

    def to_plane(d):
        return flip(z, d) if planes == 4 else (z + d) % planes

    def from_plane(d):
        return flip(z, d) if planes == 4 else (z + planes - d) % planes

    peers = (
        [(z * plane + (p + d) % plane, tp) for d in range(1, plane)]
        + [((z + d) % planes * plane + p, tp) for d in range(1, planes)]
        + [(sp, other)]
    )
    if len(widths) > 1:
        spare = widths[0] * 128
        units[:, :, spare:] = jnp.zeros((planes, tok, width - spare), jnp.bfloat16)
    barrier = pltpu.get_barrier_semaphore()
    for peer in peers:
        pl.semaphore_signal(barrier, inc=1, device_id=peer, device_id_type=MESH)

    @pl.when(tp == 1)
    def _():
        for s in range(planes):
            pl.semaphore_signal(
                barrier, inc=1, device_id=(s * plane + before, 1), device_id_type=MESH
            )

    def piece(head, row):
        h1, h2 = block_of(head, HD), block_of(head, val)
        rows, own_rows = block_of(row * plane + p, tok), block_of(row, tok)
        return [
            (k1.at[:, h1], kv_all.at[rows, 0:HD]),
            (k2.at[:, h1], kv_all.at[rows, HD : 2 * HD]),
            (v.at[:, h2], kv_all.at[rows, 2 * HD : 4 * HD]),
            (q1.at[:, h1], q_all.at[own_rows, 0:HD]),
            (q2.at[:, h1], q_all.at[own_rows, HD : 2 * HD]),
        ]


    def units_of(index, size=width):
        return pl.ds(pl.multiple_of(index * tiles // planes * 128, 128), size)

    def by_width(index, act):
        wide = (index + 1) * tiles // planes - index * tiles // planes
        for count in widths:
            if len(widths) == 1:
                act(count * 128)
            else:
                pl.when(wide == count)(functools.partial(act, count * 128))

    own = [
        pltpu.make_async_copy(src, dst, own_sem.at[n]) for n, (src, dst) in enumerate(piece(z, z))
    ]
    own_weights = [
        pltpu.make_async_copy(src.at[:, units_of(z)], dst.at[block_of(sp, tok), :], own_sem.at[5 + m])
        for m, (src, dst) in enumerate(weights)
    ]
    loads = [
        pltpu.make_async_copy(out_hbm, out_weight, own_sem.at[7]),
        pltpu.make_async_copy(residual_hbm, residual, own_sem.at[8]),
    ]

    def load(s):
        first = s * tiles // planes * 128
        return pltpu.make_async_copy(down_hbm.at[first : first + width, :], held.at[s], l_sem.at[s])

    for copy in own:
        copy.start()
    started, sized = [], []

    def send(copy):
        copy.start()
        started.append(copy)

    def send_sized(index, make):
        by_width(index, lambda size: make(size).start())
        sized.append((index, make))

    pl.semaphore_wait(barrier, len(peers) + planes * tp)

    def exchange(which):
        for d in range(1, planes):
            pairs = piece(to_plane(d), z)
            for n in which:
                src, dst = pairs[n]
                send(remote(src, dst, a_send.at[d, n], a_recv.at[d, n], to_plane(d) * plane + p, tp))

    def exchanged(d, which):
        pairs = piece(z, from_plane(d))
        for n in which:
            src, dst = pairs[n]
            remote(src, dst, a_send.at[d, n], a_recv.at[d, n], sp, other).wait_recv()

    def kv_block(d, m, chip, size):
        rows = block_of(from_plane(d) * plane + chip, tok)
        return kv_all.at[rows, m * val : (m + 1) * val]

    def weight_block(d, m, chip, size):
        return weights[m][1].at[block_of(from_plane(d) * plane + chip, tok), 0:size]

    def plain(index, make):
        send(make(width))

    kv = (kv_block, k_send, k_recv, plain, lambda index, act: act(width))
    wt = (weight_block, g_send, g_recv, send_sized, by_width)

    def spread(kind, d, m, src=None):
        block_at, sends, recvs, start, _ = kind
        for e in direct:

            def make(size, e=e):
                block = block_at(d, m, p, size)
                return remote(
                    block if src is None else src(size), block,
                    sends.at[d, e, m], recvs.at[d, e, m], z * plane + to_chip(e), tp,
                )

            start(z, make)

    def arrived(kind, d, e, m):
        block_at, sends, recvs, _, each_size = kind

        def wait(size):
            block = block_at(d, m, from_chip(e), size)
            remote(block, block, sends.at[d, e, m], recvs.at[d, e, m], sp, other).wait_recv()

        each_size(z, wait)

    def relay(kind, d, m):
        block_at, sends, recvs, start, _ = kind
        for e in direct:
            arrived(kind, d, e, m)
            if square and e == m + 1:

                def make(size, e=e):
                    block = block_at(d, m, from_chip(e), size)
                    return remote(
                        block, block, sends.at[d, 3, m], recvs.at[d, 3, m],
                        z * plane + to_chip(3 - e), tp,
                    )

                start(z, make)

    def settle(kind, d, m):
        if square:
            arrived(kind, d, 3, m)

    def send_weights(m):
        for d in range(1, planes):
            src, dst = weights[m]

            def make(size, d=d):
                return remote(
                    src.at[:, units_of(to_plane(d), size)], dst.at[block_of(sp, tok), 0:size],
                    w_send.at[d, m], w_recv.at[d, m], to_plane(d) * plane + p, tp,
                )

            send_sized(to_plane(d), make)

    def share_weights(d, m):
        if d == 0:
            spread(wt, d, m, lambda size: weights[m][0].at[:, units_of(z, size)])
            return

        def wait(size):
            block = weight_block(d, m, p, size)
            remote(block, block, w_send.at[d, m], w_recv.at[d, m], sp, other).wait_recv()

        by_width(z, wait)
        spread(wt, d, m)

    exchange((0, 1, 2))
    for copy in own[:3]:
        copy.wait()
    for m in range(2):
        spread(kv, 0, m)
    exchange((3, 4))
    share_weights(0, 0)
    send_weights(0)
    for copy in own_weights + loads:
        copy.start()
    for s in range(planes):
        load(s).start()
    for d in range(1, planes):
        exchanged(d, (0, 1, 2))
        for m in range(2):
            spread(kv, d, m)
        for m in range(2):
            relay(kv, d - 1, m)
    for m in range(2):
        relay(kv, planes - 1, m)
    share_weights(0, 1)
    relay(wt, 0, 0)
    for copy in own[3:]:
        copy.wait()
    for d in range(1, planes):
        exchanged(d, (3, 4))
    for d in range(planes):
        for m in range(2):
            settle(kv, d, m)

    for s in range(planes):
        rows, count = slice(s * tok, (s + 1) * tok), (s + 1) * span
        mixed = None
        for m in range(2):
            scores = lax.dot_general(
                q_all[rows, m * HD : (m + 1) * HD],
                kv_all[0:count, m * HD : (m + 1) * HD],
                (((1,), (1,)), ((), ())),
                preferred_element_type=jnp.float32,
            ) * HD ** (-0.5)
            k_pos = lax.broadcasted_iota(jnp.int32, (tok, span), 1)
            q_pos = p * tok + lax.broadcasted_iota(jnp.int32, (tok, span), 0)
            visible = lax.div(k_pos, STRETCH) <= lax.div(q_pos, STRETCH)
            last = jnp.where(visible, scores[:, count - span :], masked_score)
            scores = jnp.concatenate([scores[:, : count - span], last], axis=1) if s else last
            peak = jnp.max(scores, axis=-1, keepdims=True)
            terms = jnp.exp(scores - peak)
            sums = jnp.sum(terms, axis=-1, keepdims=True)
            acc = jnp.dot(
                terms.astype(jnp.bfloat16),
                kv_all[0:count, 2 * HD : 4 * HD],
                preferred_element_type=jnp.float32,
            )
            if m == 0:
                mixed = acc / sums
            else:
                mixed = mixed - mix_weight[z] * acc / sums
        scale = lax.rsqrt(jnp.mean(mixed * mixed, axis=-1, keepdims=True) + epsilon)
        head_out[s] = (mixed * scale * head_gain[...]).astype(jnp.bfloat16)

        @pl.when(z != s)
        def _():
            remote(
                head_out.at[s], heads.at[z], b_send.at[s], b_recv.at[z], s * plane + p, tp
            ).start()

        @pl.when(z == s)
        def _():
            pltpu.make_async_copy(head_out.at[s], heads.at[z], b_own).start()

    send_weights(1)
    for m in range(2):
        if m == 0:
            for d in range(1, planes):
                share_weights(d, 0)
        else:
            relay(wt, 0, 1)
    for d in range(1, planes):
        relay(wt, d, 0)
    for s in range(planes):

        @pl.when(z != s)
        def _():
            remote(
                heads.at[s], heads.at[s], b_send.at[s], b_recv.at[s], sp, other
            ).wait_recv()

        @pl.when(z == s)
        def _():
            pltpu.make_async_copy(head_out.at[s], heads.at[s], b_own).wait()

    for copy in loads:
        copy.wait()
    columns = 512

    def product(which, at):
        sums = None
        for h in range(planes):
            term = jnp.dot(
                heads[h, block_of(which, half), :],
                out_weight[h * val : (h + 1) * val, at : at + columns],
                preferred_element_type=jnp.float32,
            )
            sums = term if sums is None else sums + term
        return sums.astype(jnp.bfloat16)

    for at in range(0, model, columns):
        part[:, at : at + columns] = product(other, at)
    swap = remote(part, part_in, t_send, t_recv, sp, other)
    send(swap)
    for at in range(0, model, columns):
        stream[:, at : at + columns] = product(tp, at).astype(jnp.float32)
    swap.wait_recv()
    whole = residual[...].astype(jnp.float32) + (stream[...] + part_in[...].astype(jnp.float32))
    stream[...] = whole
    scaled = whole * lax.rsqrt(jnp.mean(whole * whole, axis=-1, keepdims=True) + epsilon) * gain[...]

    def tokens(s, which):
        return normed.at[s, pl.ds(pl.multiple_of(pad + which * half, 8), half), :]

    normed[z, pl.ds(pl.multiple_of(pad + tp * half, 8), half), :] = scaled.astype(jnp.bfloat16)
    tail[...] = scaled[half - pad :, :].astype(jnp.bfloat16)
    mine = tokens(z, tp)
    for d in range(1, planes):
        send(remote(mine, mine, n_send.at[d], n_recv.at[d], to_plane(d) * plane + p, tp))
    send(remote(mine, mine, f_send.at[0], f_recv.at[0], sp, other))

    @pl.when(jnp.logical_and(tp == 1, zone < planes))
    def _():
        for s in range(planes):
            remote(
                tail, normed.at[zone, 0:pad, :], h_send.at[s], h_recv.at[zone], s * plane + after, 1
            ).start()

    for d in range(1, planes):
        share_weights(d, 1)
    for d in range(1, planes):
        relay(wt, d, 1)

    def pass_tokens(d):
        if d:
            theirs = tokens(from_plane(d), tp)
            remote(theirs, theirs, n_send.at[d], n_recv.at[d], sp, other).wait_recv()
            send(remote(theirs, theirs, f_send.at[d], f_recv.at[d], sp, other))
        s = from_plane(d)
        rows = normed.at[s, 0:pad, :]

        @pl.when(s * plane + p > 0)
        def _():
            @pl.when(tp == 1)
            def _():
                remote(rows, rows, h_send.at[s], h_recv.at[s], sp, other).wait_recv()
                remote(rows, rows, hf_send.at[s], hf_recv.at[s], sp, other).start()

            @pl.when(tp == 0)
            def _():
                remote(rows, rows, hf_send.at[s], hf_recv.at[s], sp, other).wait_recv()

        @pl.when(s * plane + p == 0)
        def _():
            normed[s, 0:pad, :] = jnp.zeros((pad, model), jnp.bfloat16)

    pass_tokens(0)
    for copy in own_weights:
        copy.wait()
    for m in range(2):
        for d in range(planes):
            settle(wt, d, m)

    first = z * tiles // planes * 128
    mine_units = (z + 1) * tiles // planes * 128 - first
    chunk = 256 if width % 256 == 0 else 128
    for d in range(planes):
        s = from_plane(d)
        if d + 1 < planes:
            pass_tokens(d + 1)
        theirs = tokens(s, other)
        remote(theirs, theirs, f_send.at[d], f_recv.at[d], sp, other).wait_recv()

        @pl.loop(0, width // chunk)
        def _(at):
            here = block_of(at, chunk)
            gated[...] = (
                jnp.dot(normed[s], gate_all[:, here], preferred_element_type=jnp.float32)
                .astype(jnp.bfloat16)
                .astype(jnp.float32)
            )
            lifted = (
                jnp.dot(normed[s, pad:, :], lift_all[:, here], preferred_element_type=jnp.float32)
                .astype(jnp.bfloat16)
                .astype(jnp.float32)
            )
            lanes = pl.ds(pl.multiple_of(first + at * chunk, 128), chunk)
            conv = None
            for index in range(WIDTH):
                start = pad - (WIDTH - 1) + index
                term = taps[index : index + 1, lanes] * gated[start : start + tok, :]
                conv = term if conv is None else conv + term
            inside = at * chunk + lax.broadcasted_iota(jnp.int32, (tok, chunk), 1) < mine_units
            hidden[s, :, here] = jnp.where(inside, jax.nn.silu(conv) * lifted, 0.0).astype(
                jnp.bfloat16
            )

        if d:

            def make(size, s=s, d=d):
                return remote(
                    hidden.at[s, :, 0:size], units.at[z, :, 0:size],
                    u_send.at[d], u_recv.at[d], s * plane + p, tp,
                )

            send_sized(z, make)

    for d in range(planes):
        s = from_plane(d)
        if d == 0:
            for n in range(planes):
                load(n).wait()
        else:

            def wait(size, s=s, d=d):
                block = units.at[s, :, 0:size]
                remote(block, block, u_send.at[d], u_recv.at[d], sp, other).wait_recv()

            by_width(s, wait)

        @pl.loop(0, model // columns)
        def _(at):
            here = block_of(at, columns)
            block = hidden[s] if d == 0 else units[s]
            term = jnp.dot(block, held[s, :, here], preferred_element_type=jnp.float32)
            total[:, here] = term if d == 0 else total[:, here] + term

    piece_out[...] = total[block_of(other, half), :].astype(jnp.bfloat16)
    swap = remote(piece_out, piece_in, y_send, y_recv, sp, other)
    send(swap)
    near = total[block_of(tp, half), :].astype(jnp.bfloat16).astype(jnp.float32)
    swap.wait_recv()
    out[...] = (stream[...] + (near + piece_in[...].astype(jnp.float32))).astype(out.dtype)

    for s in range(planes):

        @pl.when(z != s)
        def _():
            remote(
                head_out.at[s], heads.at[z], b_send.at[s], b_recv.at[z], s * plane + p, tp
            ).wait_send()

        @pl.when(jnp.logical_and(tp == 1, s * plane + p > 0))
        def _():
            rows = normed.at[s, 0:pad, :]
            remote(rows, rows, hf_send.at[s], hf_recv.at[s], sp, other).wait_send()

        @pl.when(jnp.logical_and(tp == 1, zone < planes))
        def _():
            remote(
                tail, normed.at[s, 0:pad, :], h_send.at[s], h_recv.at[s], s * plane + after, 1
            ).wait_send()

    for copy in started:
        copy.wait_send()
    for index, make in sized:
        by_width(index, lambda size: make(size).wait_send())


def shorter_routes(
    plane, planes,
    query_one, key_one, query_two, key_two, values, mix_weight, head_gain, residual, out_weight,
    norm_gain, lift_weight, gate_weight, conv_taps, down_weight,
):
    bf16, f32 = jnp.bfloat16, jnp.float32
    tok = query_one.shape[0]
    model = residual.shape[1]
    val = 2 * HD
    tiles = lift_weight.shape[1] // 128
    width = -(-tiles // planes) * 128
    chunk = 256 if width % 256 == 0 else 128
    count = planes * plane * tok
    half = tok // 2
    pad = 8
    dma = pltpu.SemaphoreType.DMA
    anywhere = pl.BlockSpec(memory_space=pl.ANY)
    local = pl.BlockSpec(memory_space=pltpu.VMEM)
    scalars = pl.BlockSpec(memory_space=pltpu.SMEM)
    each = dma((planes,))
    return pl.pallas_call(
        functools.partial(layer_kernel, plane, planes, width),
        out_shape=jax.ShapeDtypeStruct((half, model), bf16),
        in_specs=[anywhere] * 7 + [scalars, local, anywhere, anywhere, local, local, anywhere],
        out_specs=local,
        scratch_shapes=[
            pltpu.VMEM((planes * tok, 2 * HD), bf16),
            pltpu.VMEM((count, 4 * HD), bf16),
            pltpu.VMEM((planes, tok, val), bf16),
            pltpu.VMEM((planes, tok, val), bf16),
            pltpu.VMEM((half, model), bf16),
            pltpu.VMEM((half, model), bf16),
            pltpu.VMEM((pad, model), bf16),
            pltpu.VMEM(out_weight.shape, bf16),
            pltpu.VMEM(residual.shape, bf16),
            pltpu.VMEM((half, model), f32),
            pltpu.VMEM((half, model), bf16),
            pltpu.VMEM((half, model), bf16),
            pltpu.VMEM((count, width), bf16),
            pltpu.VMEM((count, width), bf16),
            pltpu.VMEM((planes, width, model), bf16),
            pltpu.VMEM((planes, pad + tok, model), bf16),
            pltpu.VMEM((pad + tok, chunk), f32),
            pltpu.VMEM((planes, tok, width), bf16),
            pltpu.VMEM((planes, tok, width), bf16),
            pltpu.VMEM((tok, model), f32),
            dma((9,)), dma((planes, 5)), dma((planes, 5)),
            dma((planes, plane, 2)), dma((planes, plane, 2)),
            dma((planes, 2)), dma((planes, 2)),
            dma((planes, plane, 2)), dma((planes, plane, 2)), each,
            dma, each, each, dma, dma, each, each, each, each,
            each, each, each, each, each, each, dma, dma,
        ],
        compiler_params=pltpu.CompilerParams(
            collective_id=0, has_side_effects=True, vmem_limit_bytes=62 << 20
        ),
        name="layer",
    )(
        query_one, key_one, query_two, key_two, values, lift_weight, gate_weight, mix_weight,
        head_gain.reshape(1, val), out_weight, residual, norm_gain.reshape(1, model), conv_taps,
        down_weight,
    )


def any_route(*arrays):
    tok, heads, ff = arrays[0].shape[0], arrays[5].shape[0], arrays[10].shape[1]
    devices, groups = lax.axis_size("sp"), lax.axis_size("tp")
    fits = (
        groups == 2 and heads > 1 and devices > heads and devices % heads == 0
        and ff % 128 == 0 and tok % 128 == 0 and WIDTH <= 9
        and arrays[10].shape[0] == tok
    )
    if fits:
        return shorter_routes(devices // heads, heads, *arrays)
    return on_device(*arrays)


def solution(mesh):
    return jax.shard_map(
        any_route,
        mesh=mesh,
        in_specs=(
            P("sp", "tp"),
            P("sp", "tp"),
            P("sp", "tp"),
            P("sp", "tp"),
            P("sp", "tp"),
            P("tp"),
            P(),
            P(("sp", "tp"), None),
            P("tp", None),
            P(),
            P("sp", "tp"),
            P("sp", "tp"),
            P(None, "tp"),
            P("tp", None),
        ),
        out_specs=P(("sp", "tp"), None),
        check_vma=False,
    )
```
